32 devices in a mesh: ep: 8 (over z, y), tp: 4 (over x, core).
Axes of the slice: x: 2, y: 2, z: 4, core: 2. Of those that a mesh axis runs over, the one named last changes fastest.
Arguments:
- queries: bfloat16 [4096, 1024], P('ep', 'tp'), may hold values from -8 to 8
- key_rows: bfloat16 [4096, 1024], P('ep', 'tp'), may hold values from -8 to 8
- value_rows: bfloat16 [4096, 1024], P('ep', 'tp'), may hold values from -6 to 6
- lambdas: float32 [8], P('tp'), may hold values from 0.3 to 0.8
- head_gain: float32 [128], replicated, may hold values from 0.1 to 1.9
- out_weight: bfloat16 [1024, 2048], P('tp'), may hold values from -0.1875 to 0.1875
- moe_input: bfloat16 [4096, 2048], P(('ep', 'tp')), may hold values from -400 to 400
- moe_gain: float32 [2048], replicated, may hold values from 0.1 to 1.9
- routes: int32 [4096, 2], P(('ep', 'tp')), may hold values from 0 to 7, all different within a row; in each aligned block of 128 rows (0 to 127, 128 to 255, ...) at most 40 rows name the same one
- route_logits: float32 [4096, 2], P(('ep', 'tp')), may hold values from -6 to 6
- expert_gate: bfloat16 [8, 2048, 3584], P('ep', None, 'tp'), may hold values from -0.125 to 0.125
- expert_up: bfloat16 [8, 2048, 3584], P('ep', None, 'tp'), may hold values from -0.125 to 0.125
- expert_down: bfloat16 [8, 3584, 2048], P('ep', 'tp'), may hold values from -0.09375 to 0.09375
Outputs:
- mixer_out: bfloat16 [4096, 2048], P(('ep', 'tp'))
- expert_out: bfloat16 [4096, 2048], P(('ep', 'tp'))
The draws below stay inside these ranges and needn't reach their ends.
Inputs may be any that keep to these rules, and one draw needn't show every extreme that they name: `routes`: each token names 2 different experts. Among the tokens of one device no expert is named more than 40 times, and in every draw some expert is named exactly 40 times by the tokens of some device.
All inputs are finite; a program needn't handle non-finite values.
Results may differ from the reference program's by a relative error of at most 0.014.
Values may be sent and summed in bfloat16 or wider, within the bound.
A program may use at most 128 MiB of HBM per device.

```python
import math
import jax
import jax.numpy as jnp
import numpy as np
from jax import lax

D = 2048
HEADS = 8
HEAD = 64
VDIM = 128
FFE = 3584
TOP = 2
TOK2_DEV = 128
SEQ = 4096
TOKENS2 = 4096
EXPERTS = 8
CAP = 40
N_EP = 8
N_TP = 4


def drawn_pairs(key):
    folded = jax.random.fold_in(key, 17)
    key_query, key_keys = jax.random.split(folded, 2)
    row_width = HEADS * 2 * HEAD
    spread = 1.32
    query_draw = jax.random.normal(key_query, (SEQ, row_width), jnp.float32) * spread
    key_draw = jax.random.normal(key_keys, (SEQ, row_width), jnp.float32) * spread
    return (jnp.clip(query_draw, -8.0, 8.0), jnp.clip(key_draw, -8.0, 8.0))


def draw_queries(key, part):
    return drawn_pairs(key)[0].astype(jnp.bfloat16)


def draw_key_rows(key, part):
    return drawn_pairs(key)[1].astype(jnp.bfloat16)


def draw_moe_input(key, part):
    folded = jax.random.fold_in(key, 23)
    key_rows_scale, key_cols_scale, key_sample = jax.random.split(folded, 3)
    row_scale = jnp.exp(jax.random.uniform(key_rows_scale, (TOKENS2, 1), jnp.float32, 0.0, math.log(10.0)))
    column_scale = jnp.exp(jax.random.uniform(key_cols_scale, (1, D), jnp.float32, 0.0, math.log(10.0)))
    sample = jax.random.normal(key_sample, (TOKENS2, D), jnp.float32)
    return jnp.clip(sample * row_scale * column_scale, -400.0, 400.0).astype(jnp.bfloat16)


def shard_levels(key, shape, cuts, least, top_value):
    factor_of, own = 1.0, jax.random.fold_in(key, 6)
    for dim, shards_of in cuts:
        draws = jnp.exp(jax.random.uniform(jax.random.fold_in(own, dim), (shards_of,), jnp.float32, least / len(cuts), top_value / len(cuts)))
        factor_of = factor_of * jnp.repeat(draws, shape[dim] // shards_of).reshape([-1 if axis == dim else 1 for axis in range(len(shape))])
    return factor_of


def assign_block(rng, own, number, rows, count, top, most, slope):
    order = jax.random.permutation(rng, count)
    crowded, usual = shares(count, rows * top, most, slope, True), shares(count, rows * top, most, slope, False)
    places = jnp.arange(count)

    def named(lengths, rotation):
        used = int((lengths > 0).sum())
        fixed = max(1, used // 4)
        shifted = fixed + (places - fixed + rotation * (used - fixed)) % max(1, count - fixed)
        return jnp.zeros((count,), jnp.int32).at[order[jnp.where(places < fixed, places, shifted)]].set(jnp.asarray(lengths, jnp.int32))

    lengths = jnp.where(number % 4 == 0, named(crowded, number // 4), named(usual, number - number // 4 - 1))
    mixed = jax.random.permutation(jax.random.fold_in(own, 3), count)
    donor, taker = mixed[0:count // 2 * 2:2], mixed[1:count // 2 * 2:2]
    room = jnp.minimum(lengths[donor] - 1, most - lengths[taker]) // 2
    room = jnp.where((donor == order[0]) | (taker == order[0]) | (lengths[taker] == 0), 0, jnp.maximum(room, 0))
    shifted = jax.random.randint(jax.random.fold_in(own, 4), (count // 2,), 0, 1 << 20) % (room + 1)
    lengths = lengths.at[donor].add(-shifted).at[taker].add(shifted)
    items = jnp.searchsorted(jnp.cumsum(lengths), jnp.arange(rows * top), side="right").astype(jnp.int32)
    table = items.reshape(top, rows).T
    table = table[jax.random.permutation(jax.random.fold_in(own, 1), rows)]
    rotation = jax.random.randint(jax.random.fold_in(own, 2), (rows, 1), 0, top)
    return jnp.take_along_axis(table, (jnp.arange(top)[None, :] + rotation) % top, axis=1)


def shares(number_of, total, most, slope, full):
    loads = [(1 << 20) // math.isqrt(rank ** slope) + 1 for rank in range(1, number_of + 1)]
    largest = most if full else min(most, max(-(-total // number_of), total * loads[0] // sum(loads)))
    least = 1 if total - largest >= number_of - 1 else 0
    counts, rest = [largest] + [least] * (number_of - 1), total - largest - least * (number_of - 1)
    while rest > 0:
        candidates = [i for i in range(1, number_of) if counts[i] < largest] or [i for i in range(1, number_of) if counts[i] < most]
        whole, left = sum([loads[i] for i in candidates]), rest
        for i in candidates:
            more = min(most - counts[i], max(1, left * loads[i] // whole), rest)
            counts[i] = counts[i] + more
            rest = rest - more
    return np.array(counts)


def normal_values(key, dims, deviation, most, cuts=(), kind=jnp.bfloat16):
    values = deviation * jax.random.normal(key, dims, jnp.float32)
    if cuts:
        values = values * shard_levels(key, dims, cuts, -0.22, 0.18)
    return jnp.clip(values, -most, most).astype(kind)


def setup_inputs(seed: int = 0) -> dict:
    seeds = jax.random.split(jax.random.key(seed), 14)
    queries = draw_queries(jax.random.fold_in(seeds[13], 71), 0)
    key_rows = draw_key_rows(jax.random.fold_in(seeds[13], 71), 0)
    value_rows = normal_values(seeds[2], (SEQ, HEADS * VDIM), 1.0, 6.0, ((0, 8), (1, 4)))
    lambdas = jnp.clip(0.3 + 0.5 * jax.random.uniform(seeds[3], (HEADS,), jnp.float32) ** shard_levels(seeds[3], (HEADS,), ((0, 4),), -0.2, 0.2), 0.3, 0.8)
    head_gain = jnp.clip(1.0 + 0.18 * jax.random.normal(seeds[4], (VDIM,), jnp.float32), 0.1, 1.9)
    out_weight = normal_values(seeds[5], (HEADS * VDIM, D), (HEADS * VDIM) ** -0.5, 0.1875, ((0, 4),))
    moe_input = draw_moe_input(jax.random.fold_in(seeds[13], 71), 0)
    moe_gain = jnp.clip(1.0 + 0.18 * jax.random.normal(seeds[7], (D,), jnp.float32), 0.1, 1.9)
    routes_keys = jax.random.split(jax.random.fold_in(seeds[8], 1), TOKENS2 // TOK2_DEV)
    routes_turns = jax.random.permutation(jax.random.fold_in(seeds[8], 3), TOKENS2 // TOK2_DEV)
    routes = jax.vmap(lambda own, number: assign_block(jax.random.fold_in(seeds[8], 2), own, number, TOK2_DEV, EXPERTS, TOP, CAP, 1))(routes_keys, routes_turns).reshape((TOKENS2, TOP))
    route_logits = normal_values(seeds[9], (TOKENS2, TOP), 1.5, 6.0, ((0, 32),), jnp.float32)
    expert_gate = normal_values(seeds[10], (EXPERTS, D, FFE), D ** -0.5, 0.125, ((0, 8), (2, 4)))
    expert_up = normal_values(seeds[11], (EXPERTS, D, FFE), D ** -0.5, 0.125, ((0, 8), (2, 4)))
    expert_down = normal_values(seeds[12], (EXPERTS, FFE, D), FFE ** -0.5, 0.09375, ((0, 8), (1, 4)))
    return dict(queries=queries, key_rows=key_rows, value_rows=value_rows, lambdas=lambdas, head_gain=head_gain, out_weight=out_weight, moe_input=moe_input, moe_gain=moe_gain, routes=routes, route_logits=route_logits, expert_gate=expert_gate, expert_up=expert_up, expert_down=expert_down)


epsilon = 1e-06
init_lambda = 0.2

def one_head(query_head, key_head, value_head, lambda_head, head_gain):
    seq_len = query_head.shape[0]
    block_rows = math.gcd(seq_len, 512)
    score_scale = HEAD ** (-0.5)
    blocks = query_head.reshape(seq_len // block_rows, block_rows, 2, HEAD)

    def one_block(query_block):
        outputs = []
        for map_index in range(2):
            scores = jnp.dot(query_block[:, map_index], key_head[:, map_index].T, preferred_element_type=jnp.float32) * score_scale
            maxima = lax.optimization_barrier(jnp.max(scores, axis=-1, keepdims=True))
            exponent = jnp.exp(scores - maxima)
            totals = lax.optimization_barrier(jnp.sum(exponent, axis=-1, keepdims=True))
            product = jnp.dot(exponent.astype(jnp.bfloat16), value_head, preferred_element_type=jnp.float32)
            outputs.append(product / totals)
        head_out = outputs[0] - lambda_head * outputs[1]
        mean_square = lax.optimization_barrier(jnp.mean(head_out * head_out, axis=-1, keepdims=True))
        return (head_out * lax.rsqrt(mean_square + epsilon) * head_gain * (1.0 - init_lambda)).astype(jnp.bfloat16)
    return lax.map(one_block, blocks).reshape(seq_len, VDIM)

def reference(queries, key_rows, value_rows, lambdas, head_gain, out_weight, moe_input, moe_gain, routes, route_logits, expert_gate, expert_up, expert_down):
    seq_len = queries.shape[0]
    query_heads = queries.reshape(seq_len, HEADS, 2, HEAD).transpose(1, 0, 2, 3)
    key_heads = key_rows.reshape(seq_len, HEADS, 2, HEAD).transpose(1, 0, 2, 3)
    value_heads = value_rows.reshape(seq_len, HEADS, VDIM).transpose(1, 0, 2)

    def head_step(packed):
        return one_head(packed[0], packed[1], packed[2], packed[3], head_gain)
    attended = lax.map(head_step, (query_heads, key_heads, value_heads, lambdas))
    group_heads = HEADS // N_TP
    weight_heads = out_weight.reshape(HEADS, VDIM, D)
    mixer_total = jnp.zeros((seq_len, D), jnp.float32)
    for group_index in range(N_TP):
        lower = group_index * group_heads
        partial_value = jnp.einsum('hqe,hed->qd', attended[lower:lower + group_heads].astype(jnp.float32), weight_heads[lower:lower + group_heads].astype(jnp.float32))
        mixer_total = mixer_total + lax.optimization_barrier(partial_value.astype(jnp.bfloat16)).astype(jnp.float32)
    mixer_out = mixer_total.astype(jnp.bfloat16)
    moe_float = moe_input.astype(jnp.float32)
    normed = (moe_float * lax.rsqrt(lax.optimization_barrier(jnp.mean(moe_float * moe_float, axis=-1, keepdims=True)) + epsilon) * moe_gain).astype(jnp.bfloat16)
    gate_weights = jax.nn.softmax(route_logits, axis=-1)
    device_count = N_EP * N_TP
    per_device = TOK2_DEV * TOP
    flat_routes = routes.reshape(device_count, per_device)
    chosen = (flat_routes[:, :, None] == jnp.arange(EXPERTS, dtype=jnp.int32)[None, None, :]).astype(jnp.int32)
    slot_rank = lax.optimization_barrier(jnp.sum((jnp.cumsum(chosen, axis=1) - chosen) * chosen, axis=2))
    device_ids = jnp.arange(device_count, dtype=jnp.int32)[:, None] * jnp.ones((1, per_device), jnp.int32)
    positions = (device_ids * CAP + slot_rank).reshape(-1).astype(jnp.int32)
    row_ids = (jnp.arange(device_count * per_device, dtype=jnp.int32) // TOP).astype(jnp.int32)
    expert_ids = flat_routes.reshape(-1).astype(jnp.int32)
    slot_table = jnp.full((EXPERTS, device_count * CAP), TOKENS2, jnp.int32).at[expert_ids, positions].set(row_ids)
    padded = jnp.concatenate([normed, jnp.zeros((1, D), jnp.bfloat16)], axis=0)
    width_part = FFE // N_TP

    def one_expert(packed):
        indices, gate_matrix, up_matrix, down_matrix = packed
        rows_in = padded[indices]
        gate_part = jnp.dot(rows_in, gate_matrix, preferred_element_type=jnp.float32)
        up_part = jnp.dot(rows_in, up_matrix, preferred_element_type=jnp.float32)
        hidden = (jax.nn.silu(gate_part) * up_part).astype(jnp.bfloat16)
        summed = jnp.zeros((rows_in.shape[0], D), jnp.float32)
        for group_index in range(N_TP):
            lower = group_index * width_part
            partial_value = jnp.dot(hidden[:, lower:lower + width_part], down_matrix[lower:lower + width_part], preferred_element_type=jnp.float32)
            summed = summed + lax.optimization_barrier(partial_value.astype(jnp.bfloat16)).astype(jnp.float32)
        return summed.astype(jnp.bfloat16)
    replies = lax.map(one_expert, (slot_table, expert_gate, expert_up, expert_down))
    picked = replies[expert_ids, positions].reshape(TOKENS2, TOP, D)
    expert_out = lax.optimization_barrier(jnp.sum(gate_weights[:, :, None] * picked.astype(jnp.float32), axis=1)).astype(jnp.bfloat16)
    return (mixer_out, expert_out)
```

```python
import functools

import jax
import jax.numpy as jnp
from jax import lax
from jax.experimental import pallas as pl
from jax.experimental.pallas import tpu as pltpu
from jax.sharding import PartitionSpec as P

MESH = pl.DeviceIdType.MESH

epsilon = 1e-06
init_lambda = 0.2


def capacity(tokens, top_count, experts):
    return max(2, (top_count * tokens * 5 + 4 * experts - 1) // (4 * experts))


def positions(experts_all, groups):
    me, tp = lax.axis_index("ep"), lax.axis_index("tp")
    near = tp + 1 - 2 * lax.rem(tp, 2)
    far = lax.rem(tp + groups // 2, groups)
    return me, tp, near, far


def greet(experts_all, me, tp, near, far):
    barrier = pltpu.get_barrier_semaphore()
    for shift in range(1, experts_all):
        pl.semaphore_signal(
            barrier, inc=1, device_id=(lax.rem(me + shift, experts_all), tp), device_id_type=MESH
        )
    for peer in (near, far):
        pl.semaphore_signal(barrier, inc=1, device_id=(me, peer), device_id_type=MESH)
    pl.semaphore_wait(barrier, experts_all + 1)


def spread_kernel(
    experts_all, groups, outgoing, segment, own_sem, send_sems, recv_sems
):
    me, tp, near, far = positions(experts_all, groups)
    greet(experts_all, me, tp, near, far)

    def copy(kind, shift, source, target, place):
        return pltpu.make_async_remote_copy(
            src_ref=source,
            dst_ref=target,
            send_sem=send_sems.at[kind, shift],
            recv_sem=recv_sems.at[kind, shift],
            device_id=place,
            device_id_type=MESH,
        )

    own = pltpu.make_async_copy(outgoing.at[me], segment.at[tp, me], own_sem)
    own.start()
    arrivals = {}
    for shift in range(1, experts_all):
        there = lax.rem(me + shift, experts_all)
        arrivals[shift] = copy(0, shift, outgoing.at[there], segment.at[tp, me], (there, tp))
        arrivals[shift].start()
    near_copies, far_copies, relayed = {}, {}, {}
    own.wait()
    for shift in range(experts_all):
        block = segment.at[tp, lax.rem(me + experts_all - shift, experts_all)]
        if shift:
            arrivals[shift].wait_recv()
        far_copies[shift] = copy(2, shift, block, block, (me, far))
        far_copies[shift].start()
        near_copies[shift] = copy(1, shift, block, block, (me, near))
        near_copies[shift].start()
    for shift in range(experts_all):
        block = segment.at[far, lax.rem(me + experts_all - shift, experts_all)]
        far_copies[shift].wait_recv()
        relayed[shift] = copy(3, shift, block, block, (me, near))
        relayed[shift].start()
    for shift in range(experts_all):
        near_copies[shift].wait_recv()
        relayed[shift].wait_recv()
    for shift in range(experts_all):
        if shift:
            arrivals[shift].wait_send()
        near_copies[shift].wait_send()
        far_copies[shift].wait_send()
        relayed[shift].wait_send()


def spread(outgoing, groups):
    experts_all, slot_count, width = outgoing.shape
    return pl.pallas_call(
        functools.partial(spread_kernel, experts_all, groups),
        out_shape=jax.ShapeDtypeStruct((groups,) + outgoing.shape, outgoing.dtype),
        in_specs=[pl.BlockSpec(memory_space=pltpu.VMEM)],
        out_specs=pl.BlockSpec(memory_space=pl.ANY),
        scratch_shapes=[
            pltpu.SemaphoreType.DMA,
            pltpu.SemaphoreType.DMA((4, experts_all)),
            pltpu.SemaphoreType.DMA((4, experts_all)),
        ],
        compiler_params=pltpu.CompilerParams(collective_id=0, has_side_effects=True),
        cost_estimate=pl.CostEstimate(
            flops=40_000_000_000, bytes_accessed=2 * outgoing.size, transcendentals=0
        ),
        name="spread",
    )(outgoing)


def gather_kernel(
    experts_all,
    groups,
    parts,
    replies,
    near_in,
    pair_out,
    far_in,
    reply_out,
    own_sem,
    send_sems,
    recv_sems,
):
    me, tp, near, far = positions(experts_all, groups)
    near_far = lax.rem(near + groups // 2, groups)
    greet(experts_all, me, tp, near, far)

    def copy(kind, shift, source, target, place):
        return pltpu.make_async_remote_copy(
            src_ref=source,
            dst_ref=target,
            send_sem=send_sems.at[kind, shift],
            recv_sem=recv_sems.at[kind, shift],
            device_id=place,
            device_id_type=MESH,
        )

    order = list(range(1, experts_all)) + [0]
    blocks = [lax.rem(me + shift, experts_all) for shift in range(experts_all)]
    pair_copies, near_copies, far_copies, back = {}, {}, {}, {}
    for shift in order:
        block = blocks[shift]
        pair_copies[shift] = copy(
            0, shift, parts.at[near_far, block], near_in.at[1, block], (me, near)
        )
        pair_copies[shift].start()
    for shift in order:
        block = blocks[shift]
        near_copies[shift] = copy(1, shift, parts.at[near, block], near_in.at[0, block], (me, near))
        near_copies[shift].start()
    for shift in order:
        block = blocks[shift]
        pair_copies[shift].wait_recv()
        pair_out[block] = (
            parts[far, block].astype(jnp.float32) + near_in[1, block].astype(jnp.float32)
        ).astype(jnp.bfloat16)
        far_copies[shift] = copy(2, shift, pair_out.at[block], far_in.at[block], (me, far))
        far_copies[shift].start()
    for shift in order:
        block = blocks[shift]
        near_copies[shift].wait_recv()
        far_copies[shift].wait_recv()
        reply_out[block] = (
            parts[tp, block].astype(jnp.float32)
            + near_in[0, block].astype(jnp.float32)
            + far_in[block].astype(jnp.float32)
        ).astype(jnp.bfloat16)
        if shift:
            back[shift] = copy(3, shift, reply_out.at[block], replies.at[me], (block, tp))
        else:
            back[shift] = pltpu.make_async_copy(reply_out.at[me], replies.at[me], own_sem)
        back[shift].start()
    for shift in order:
        back[shift].wait()
        pair_copies[shift].wait_send()
        near_copies[shift].wait_send()
        far_copies[shift].wait_send()


def gather_replies(parts):
    groups, experts_all = parts.shape[:2]
    one_group = parts.shape[1:]
    return pl.pallas_call(
        functools.partial(gather_kernel, experts_all, groups),
        out_shape=jax.ShapeDtypeStruct(one_group, parts.dtype),
        in_specs=[pl.BlockSpec(memory_space=pltpu.VMEM)],
        out_specs=pl.BlockSpec(memory_space=pl.ANY),
        scratch_shapes=[
            pltpu.VMEM((2,) + one_group, parts.dtype),
            pltpu.VMEM(one_group, parts.dtype),
            pltpu.VMEM(one_group, parts.dtype),
            pltpu.VMEM(one_group, parts.dtype),
            pltpu.SemaphoreType.DMA,
            pltpu.SemaphoreType.DMA((4, experts_all)),
            pltpu.SemaphoreType.DMA((4, experts_all)),
        ],
        compiler_params=pltpu.CompilerParams(
            collective_id=1, has_side_effects=True, vmem_limit_bytes=40 * 2**20
        ),
        cost_estimate=pl.CostEstimate(
            flops=40_000_000_000, bytes_accessed=2 * parts.size, transcendentals=0
        ),
        name="gather_replies",
    )(parts)


def per_device(
    queries,
    key_rows,
    value_rows,
    lambdas,
    head_gain,
    out_weight,
    moe_input,
    moe_gain,
    routes,
    route_logits,
    expert_gate,
    expert_up,
    expert_down,
):
    local_rows = queries.shape[0]
    local_heads = lambdas.shape[0]
    head_size = queries.shape[1] // (2 * local_heads)
    value_size = value_rows.shape[1] // local_heads
    model_width = out_weight.shape[1]
    score_scale = head_size ** (-0.5)
    query_maps = queries.reshape(local_rows, local_heads, 2, head_size)

    def attend_block(running, key_block, value_block):
        maxima, totals, accumulated = running
        key_count = key_block.shape[0]
        key_maps = key_block.reshape(key_count, local_heads, 2, head_size)
        value_heads = value_block.reshape(key_count, local_heads, value_size)
        scores = (
            jnp.einsum("qhid,khid->ihqk", query_maps, key_maps, preferred_element_type=jnp.float32)
            * score_scale
        )
        new_max = jnp.maximum(maxima, jnp.max(scores, axis=-1))
        weights = jnp.exp(scores - new_max[..., None])
        factor = jnp.exp(maxima - new_max)
        totals = totals * factor + jnp.sum(weights, axis=-1)
        accumulated = accumulated * factor[..., None] + jnp.einsum(
            "ihqk,khe->ihqe",
            weights.astype(jnp.bfloat16),
            value_heads,
            preferred_element_type=jnp.float32,
        )
        return (new_max, totals, accumulated)

    initial = (
        jnp.full((2, local_heads, local_rows), -1e30, jnp.float32),
        jnp.zeros((2, local_heads, local_rows), jnp.float32),
        jnp.zeros((2, local_heads, local_rows, value_size), jnp.float32),
    )
    key_piece = lax.all_gather(key_rows, "ep", axis=0, tiled=True)
    value_piece = lax.all_gather(value_rows, "ep", axis=0, tiled=True)
    length = key_piece.shape[0]
    block_rows = length
    while block_rows > 1024 and block_rows % 2 == 0:
        block_rows //= 2

    def loop_body(step_index, partial_state):
        first_row = step_index * block_rows
        return attend_block(
            partial_state,
            lax.dynamic_slice_in_dim(key_piece, first_row, block_rows, 0),
            lax.dynamic_slice_in_dim(value_piece, first_row, block_rows, 0),
        )

    maxima, totals, accumulated = lax.fori_loop(0, length // block_rows, loop_body, initial)
    maps_out = accumulated / totals[..., None]
    head_out = maps_out[0] - lambdas[:, None, None] * maps_out[1]
    mean_square = jnp.mean(head_out * head_out, axis=-1, keepdims=True)
    attended = (
        head_out * lax.rsqrt(mean_square + epsilon) * head_gain * (1.0 - init_lambda)
    ).astype(jnp.bfloat16)
    out_heads = out_weight.reshape(local_heads, value_size, model_width)
    token_count, top_count = routes.shape
    experts_all = lax.axis_size("ep")
    groups = lax.axis_size("tp")
    slot_count = -(-capacity(token_count, top_count, experts_all) // 8) * 8
    moe_float = moe_input.astype(jnp.float32)
    normed = (
        moe_float
        * lax.rsqrt(jnp.mean(moe_float * moe_float, axis=-1, keepdims=True) + epsilon)
        * moe_gain
    ).astype(jnp.bfloat16)
    gate_weights = jax.nn.softmax(route_logits, axis=-1)
    flat_routes = routes.reshape(-1)
    chosen = (flat_routes[:, None] == jnp.arange(experts_all, dtype=jnp.int32)[None, :]).astype(
        jnp.int32
    )
    slot_rank = jnp.sum((jnp.cumsum(chosen, axis=0) - chosen) * chosen, axis=1)
    slot_ids = (flat_routes * slot_count + slot_rank).reshape(token_count, top_count)
    dispatch = jnp.any(
        slot_ids[None, :, :]
        == jnp.arange(experts_all * slot_count, dtype=jnp.int32)[:, None, None],
        axis=-1,
    ).astype(jnp.bfloat16)
    outgoing = (
        jnp.dot(dispatch, normed, preferred_element_type=jnp.float32)
        .astype(jnp.bfloat16)
        .reshape(experts_all, slot_count, model_width)
    )
    gate_local = expert_gate[0]
    up_local = expert_up[0]
    down_local = expert_down[0]
    segment = spread(outgoing, groups).reshape(groups * experts_all * slot_count, model_width)
    gate_part = jnp.dot(segment, gate_local, preferred_element_type=jnp.float32)
    up_part = jnp.dot(segment, up_local, preferred_element_type=jnp.float32)
    hidden = (jax.nn.silu(gate_part) * up_part).astype(jnp.bfloat16)
    expert_slots = experts_all * slot_count
    mixer_sum = lax.psum_scatter(
        jnp.einsum("hqe,hed->qd", attended, out_heads, preferred_element_type=jnp.float32).astype(
            jnp.bfloat16
        ),
        "tp",
        scatter_dimension=0,
        tiled=True,
    )
    parts = jnp.dot(hidden, down_local, preferred_element_type=jnp.float32).astype(jnp.bfloat16)
    replies = gather_replies(
        parts.reshape(groups, experts_all, slot_count, model_width)
    ).reshape(expert_slots, model_width)
    places = jnp.arange(expert_slots, dtype=jnp.int32)
    combine = jnp.sum(
        jnp.where(slot_ids[:, :, None] == places[None, None, :], gate_weights[:, :, None], 0.0),
        axis=1,
    )
    combine_high = combine.astype(jnp.bfloat16)
    combine_low = (combine - combine_high.astype(jnp.float32)).astype(jnp.bfloat16)
    expert_out = (
        jnp.dot(combine_high, replies, preferred_element_type=jnp.float32)
        + jnp.dot(combine_low, replies, preferred_element_type=jnp.float32)
    ).astype(jnp.bfloat16)
    return (mixer_sum, expert_out)


def solution(mesh):
    placed = (
        P("ep", "tp"),
        P("ep", "tp"),
        P("ep", "tp"),
        P("tp"),
        P(),
        P("tp", None),
        P(("ep", "tp"), None),
        P(),
        P(("ep", "tp"), None),
        P(("ep", "tp"), None),
        P("ep", None, "tp"),
        P("ep", None, "tp"),
        P("ep", "tp", None),
    )
    return jax.shard_map(
        per_device,
        mesh=mesh,
        in_specs=placed,
        out_specs=(P(("ep", "tp"), None), P(("ep", "tp"), None)),
        check_vma=False,
    )
```

```python
import functools

import jax
import jax.numpy as jnp
from jax import lax
from jax.experimental import pallas as pl
from jax.experimental.pallas import tpu as pltpu
from jax.sharding import PartitionSpec as P

MESH = pl.DeviceIdType.MESH

epsilon = 1e-06
init_lambda = 0.2


def capacity(tokens, top_count, experts):
    return max(2, (top_count * tokens * 5 + 4 * experts - 1) // (4 * experts))


def positions(experts_all, groups):
    me, tp = lax.axis_index("ep"), lax.axis_index("tp")
    near = tp + 1 - 2 * lax.rem(tp, 2)
    far = lax.rem(tp + groups // 2, groups)
    return me, tp, near, far


def greet(experts_all, me, tp, near, far):
    barrier = pltpu.get_barrier_semaphore()
    for shift in range(1, experts_all):
        pl.semaphore_signal(
            barrier, inc=1, device_id=(lax.rem(me + shift, experts_all), tp), device_id_type=MESH
        )
    for peer in (near, far):
        pl.semaphore_signal(barrier, inc=1, device_id=(me, peer), device_id_type=MESH)
    pl.semaphore_wait(barrier, experts_all + 1)


def spread_kernel(
    experts_all, groups, outgoing, segment, own_sem, send_sems, recv_sems
):
    me, tp, near, far = positions(experts_all, groups)
    greet(experts_all, me, tp, near, far)

    def copy(kind, shift, source, target, place):
        return pltpu.make_async_remote_copy(
            src_ref=source,
            dst_ref=target,
            send_sem=send_sems.at[kind, shift],
            recv_sem=recv_sems.at[kind, shift],
            device_id=place,
            device_id_type=MESH,
        )

    own = pltpu.make_async_copy(outgoing.at[me], segment.at[tp, me], own_sem)
    own.start()
    arrivals = {}
    for shift in range(1, experts_all):
        there = lax.rem(me + shift, experts_all)
        arrivals[shift] = copy(0, shift, outgoing.at[there], segment.at[tp, me], (there, tp))
        arrivals[shift].start()
    near_copies, far_copies, relayed = {}, {}, {}
    own.wait()
    for shift in range(experts_all):
        block = segment.at[tp, lax.rem(me + experts_all - shift, experts_all)]
        if shift:
            arrivals[shift].wait_recv()
        far_copies[shift] = copy(2, shift, block, block, (me, far))
        far_copies[shift].start()
        near_copies[shift] = copy(1, shift, block, block, (me, near))
        near_copies[shift].start()
    for shift in range(experts_all):
        block = segment.at[far, lax.rem(me + experts_all - shift, experts_all)]
        far_copies[shift].wait_recv()
        relayed[shift] = copy(3, shift, block, block, (me, near))
        relayed[shift].start()
    for shift in range(experts_all):
        near_copies[shift].wait_recv()
        relayed[shift].wait_recv()
    for shift in range(experts_all):
        if shift:
            arrivals[shift].wait_send()
        near_copies[shift].wait_send()
        far_copies[shift].wait_send()
        relayed[shift].wait_send()


def spread(outgoing, groups):
    experts_all, slot_count, width = outgoing.shape
    return pl.pallas_call(
        functools.partial(spread_kernel, experts_all, groups),
        out_shape=jax.ShapeDtypeStruct((groups,) + outgoing.shape, outgoing.dtype),
        in_specs=[pl.BlockSpec(memory_space=pltpu.VMEM)],
        out_specs=pl.BlockSpec(memory_space=pl.ANY),
        scratch_shapes=[
            pltpu.SemaphoreType.DMA,
            pltpu.SemaphoreType.DMA((4, experts_all)),
            pltpu.SemaphoreType.DMA((4, experts_all)),
        ],
        compiler_params=pltpu.CompilerParams(collective_id=0, has_side_effects=True),
        cost_estimate=pl.CostEstimate(
            flops=40_000_000_000, bytes_accessed=2 * outgoing.size, transcendentals=0
        ),
        name="spread",
    )(outgoing)


def gather_kernel(
    experts_all,
    groups,
    parts,
    replies,
    near_in,
    pair_out,
    far_in,
    reply_out,
    own_sem,
    send_sems,
    recv_sems,
):
    me, tp, near, far = positions(experts_all, groups)
    near_far = lax.rem(near + groups // 2, groups)
    greet(experts_all, me, tp, near, far)

    def copy(kind, shift, source, target, place):
        return pltpu.make_async_remote_copy(
            src_ref=source,
            dst_ref=target,
            send_sem=send_sems.at[kind, shift],
            recv_sem=recv_sems.at[kind, shift],
            device_id=place,
            device_id_type=MESH,
        )

    order = list(range(1, experts_all)) + [0]
    blocks = [lax.rem(me + shift, experts_all) for shift in range(experts_all)]
    pair_copies, near_copies, far_copies, back = {}, {}, {}, {}
    for shift in order:
        block = blocks[shift]
        pair_copies[shift] = copy(
            0, shift, parts.at[near_far, block], near_in.at[1, block], (me, near)
        )
        pair_copies[shift].start()
    for shift in order:
        block = blocks[shift]
        near_copies[shift] = copy(1, shift, parts.at[near, block], near_in.at[0, block], (me, near))
        near_copies[shift].start()
    for shift in order:
        block = blocks[shift]
        pair_copies[shift].wait_recv()
        pair_out[block] = (
            parts[far, block].astype(jnp.float32) + near_in[1, block].astype(jnp.float32)
        ).astype(jnp.bfloat16)
        far_copies[shift] = copy(2, shift, pair_out.at[block], far_in.at[block], (me, far))
        far_copies[shift].start()
    for shift in order:
        block = blocks[shift]
        near_copies[shift].wait_recv()
        far_copies[shift].wait_recv()
        reply_out[block] = (
            parts[tp, block].astype(jnp.float32)
            + near_in[0, block].astype(jnp.float32)
            + far_in[block].astype(jnp.float32)
        ).astype(jnp.bfloat16)
        if shift:
            back[shift] = copy(3, shift, reply_out.at[block], replies.at[me], (block, tp))
        else:
            back[shift] = pltpu.make_async_copy(reply_out.at[me], replies.at[me], own_sem)
        back[shift].start()
    for shift in order:
        back[shift].wait()
        pair_copies[shift].wait_send()
        near_copies[shift].wait_send()
        far_copies[shift].wait_send()


def gather_replies(parts):
    groups, experts_all = parts.shape[:2]
    one_group = parts.shape[1:]
    return pl.pallas_call(
        functools.partial(gather_kernel, experts_all, groups),
        out_shape=jax.ShapeDtypeStruct(one_group, parts.dtype),
        in_specs=[pl.BlockSpec(memory_space=pltpu.VMEM)],
        out_specs=pl.BlockSpec(memory_space=pl.ANY),
        scratch_shapes=[
            pltpu.VMEM((2,) + one_group, parts.dtype),
            pltpu.VMEM(one_group, parts.dtype),
            pltpu.VMEM(one_group, parts.dtype),
            pltpu.VMEM(one_group, parts.dtype),
            pltpu.SemaphoreType.DMA,
            pltpu.SemaphoreType.DMA((4, experts_all)),
            pltpu.SemaphoreType.DMA((4, experts_all)),
        ],
        compiler_params=pltpu.CompilerParams(
            collective_id=1, has_side_effects=True, vmem_limit_bytes=40 * 2**20
        ),
        cost_estimate=pl.CostEstimate(
            flops=40_000_000_000, bytes_accessed=2 * parts.size, transcendentals=0
        ),
        name="gather_replies",
    )(parts)


def per_device(
    queries,
    key_rows,
    value_rows,
    lambdas,
    head_gain,
    out_weight,
    moe_input,
    moe_gain,
    routes,
    route_logits,
    expert_gate,
    expert_up,
    expert_down,
):
    local_rows = queries.shape[0]
    local_heads = lambdas.shape[0]
    head_size = queries.shape[1] // (2 * local_heads)
    value_size = value_rows.shape[1] // local_heads
    model_width = out_weight.shape[1]
    score_scale = head_size ** (-0.5)
    query_maps = queries.reshape(local_rows, local_heads, 2, head_size)

    def attend_block(running, key_block, value_block):
        maxima, totals, accumulated = running
        key_count = key_block.shape[0]
        key_maps = key_block.reshape(key_count, local_heads, 2, head_size)
        value_heads = value_block.reshape(key_count, local_heads, value_size)
        scores = (
            jnp.einsum("qhid,khid->ihqk", query_maps, key_maps, preferred_element_type=jnp.float32)
            * score_scale
        )
        new_max = jnp.maximum(maxima, jnp.max(scores, axis=-1))
        weights = jnp.exp(scores - new_max[..., None])
        factor = jnp.exp(maxima - new_max)
        totals = totals * factor + jnp.sum(weights, axis=-1)
        accumulated = accumulated * factor[..., None] + jnp.einsum(
            "ihqk,khe->ihqe",
            weights.astype(jnp.bfloat16),
            value_heads,
            preferred_element_type=jnp.float32,
        )
        return (new_max, totals, accumulated)

    initial = (
        jnp.full((2, local_heads, local_rows), -1e30, jnp.float32),
        jnp.zeros((2, local_heads, local_rows), jnp.float32),
        jnp.zeros((2, local_heads, local_rows, value_size), jnp.float32),
    )
    key_piece = lax.all_gather(key_rows, "ep", axis=0, tiled=True)
    value_piece = lax.all_gather(value_rows, "ep", axis=0, tiled=True)
    length = key_piece.shape[0]
    block_rows = length
    while block_rows > 1024 and block_rows % 2 == 0:
        block_rows //= 2

    def loop_body(step_index, partial_state):
        first_row = step_index * block_rows
        return attend_block(
            partial_state,
            lax.dynamic_slice_in_dim(key_piece, first_row, block_rows, 0),
            lax.dynamic_slice_in_dim(value_piece, first_row, block_rows, 0),
        )

    token_count, top_count = routes.shape
    experts_all = lax.axis_size("ep")
    groups = lax.axis_size("tp")
    slot_count = -(-capacity(token_count, top_count, experts_all) // 8) * 8
    moe_float = moe_input.astype(jnp.float32)
    normed = (
        moe_float
        * lax.rsqrt(jnp.mean(moe_float * moe_float, axis=-1, keepdims=True) + epsilon)
        * moe_gain
    ).astype(jnp.bfloat16)
    gate_weights = jax.nn.softmax(route_logits, axis=-1)
    flat_routes = routes.reshape(-1)
    chosen = (flat_routes[:, None] == jnp.arange(experts_all, dtype=jnp.int32)[None, :]).astype(
        jnp.int32
    )
    slot_rank = jnp.sum((jnp.cumsum(chosen, axis=0) - chosen) * chosen, axis=1)
    slot_ids = (flat_routes * slot_count + slot_rank).reshape(token_count, top_count)
    dispatch = jnp.any(
        slot_ids[None, :, :]
        == jnp.arange(experts_all * slot_count, dtype=jnp.int32)[:, None, None],
        axis=-1,
    ).astype(jnp.bfloat16)
    outgoing = (
        jnp.dot(dispatch, normed, preferred_element_type=jnp.float32)
        .astype(jnp.bfloat16)
        .reshape(experts_all, slot_count, model_width)
    )
    gate_local = expert_gate[0]
    up_local = expert_up[0]
    down_local = expert_down[0]
    segment = spread(outgoing, groups).reshape(groups * experts_all * slot_count, model_width)
    gate_part = jnp.dot(segment, gate_local, preferred_element_type=jnp.float32)
    up_part = jnp.dot(segment, up_local, preferred_element_type=jnp.float32)
    hidden = (jax.nn.silu(gate_part) * up_part).astype(jnp.bfloat16)
    expert_slots = experts_all * slot_count
    parts = jnp.dot(hidden, down_local, preferred_element_type=jnp.float32).astype(jnp.bfloat16)
    replies = gather_replies(
        parts.reshape(groups, experts_all, slot_count, model_width)
    ).reshape(expert_slots, model_width)
    replies, initial = lax.optimization_barrier((replies, initial))
    maxima, totals, accumulated = lax.fori_loop(0, length // block_rows, loop_body, initial)
    maps_out = accumulated / totals[..., None]
    head_out = maps_out[0] - lambdas[:, None, None] * maps_out[1]
    mean_square = jnp.mean(head_out * head_out, axis=-1, keepdims=True)
    attended = (
        head_out * lax.rsqrt(mean_square + epsilon) * head_gain * (1.0 - init_lambda)
    ).astype(jnp.bfloat16)
    out_heads = out_weight.reshape(local_heads, value_size, model_width)
    mixer_sum = lax.psum_scatter(
        jnp.einsum("hqe,hed->qd", attended, out_heads, preferred_element_type=jnp.float32).astype(
            jnp.bfloat16
        ),
        "tp",
        scatter_dimension=0,
        tiled=True,
    )
    places = jnp.arange(expert_slots, dtype=jnp.int32)
    combine = jnp.sum(
        jnp.where(slot_ids[:, :, None] == places[None, None, :], gate_weights[:, :, None], 0.0),
        axis=1,
    )
    combine_high = combine.astype(jnp.bfloat16)
    combine_low = (combine - combine_high.astype(jnp.float32)).astype(jnp.bfloat16)
    expert_out = (
        jnp.dot(combine_high, replies, preferred_element_type=jnp.float32)
        + jnp.dot(combine_low, replies, preferred_element_type=jnp.float32)
    ).astype(jnp.bfloat16)
    return (mixer_sum, expert_out)


def solution(mesh):
    placed = (
        P("ep", "tp"),
        P("ep", "tp"),
        P("ep", "tp"),
        P("tp"),
        P(),
        P("tp", None),
        P(("ep", "tp"), None),
        P(),
        P(("ep", "tp"), None),
        P(("ep", "tp"), None),
        P("ep", None, "tp"),
        P("ep", None, "tp"),
        P("ep", "tp", None),
    )
    return jax.shard_map(
        per_device,
        mesh=mesh,
        in_specs=placed,
        out_specs=(P(("ep", "tp"), None), P(("ep", "tp"), None)),
        check_vma=False,
    )
```
